32 devices in a mesh: ep: 8 (over z, x), tp: 4 (over y, core).
Axes of the slice: x: 2, y: 2, z: 4, core: 2. Of those that a mesh axis runs over, the one named last changes fastest.
Arguments:
- gate_branch: bfloat16 [4096, 2048], P(('ep', 'tp')), may hold values from -8 to 8
- rec_branch: bfloat16 [4096, 2048], P(('ep', 'tp')), may hold values from -6 to 6
- conv_weight: float32 [4, 2048], replicated, may hold values from -3 to 3
- gate_a: bfloat16 [8, 256, 256], replicated, may hold values from -0.375 to 0.375
- gate_x: bfloat16 [8, 256, 256], replicated, may hold values from -0.375 to 0.375
- decay_param: float32 [2048], replicated, as said below
- decay_shift: float32 [4096], P(('ep', 'tp')), may hold values from -0.6 to 0
- tokens: bfloat16 [4096, 2048], P(('ep', 'tp')), may hold values from -6 to 6
- routes: int32 [4096, 2], P(('ep', 'tp')), may hold values from 0 to 7, all different within a row; in each aligned block of 128 rows (0 to 127, 128 to 255, ...) at most 40 rows name the same one
- route_weight: float32 [4096, 2], P(('ep', 'tp')), may hold values from 0.1 to 0.9
- norm_gain: float32 [2048], replicated, may hold values from 0.1 to 1.9
- w_gate: bfloat16 [8, 2048, 3584], P('ep', None, 'tp'), may hold values from -0.125 to 0.125
- w_up: bfloat16 [8, 2048, 3584], P('ep', None, 'tp'), may hold values from -0.125 to 0.125
- w_down: bfloat16 [8, 3584, 2048], P('ep', 'tp'), may hold values from -0.09375 to 0.09375
Outputs:
- mixed_out: bfloat16 [4096, 2048], P(('ep', 'tp'))
- expert_out: bfloat16 [4096, 2048], P(('ep', 'tp'))
The draws below stay inside these ranges and needn't reach their ends.
Inputs may be any that keep to these rules, and one draw needn't show every extreme that they name: `routes`: in each aligned block of 128 rows (the rows of one device) no expert is named more than 40 times, and some block names some expert exactly 40 times; the experts of one row differ. 8 softplus(-decay_param) lies between 0.2 / 4096 and 0.07.
All inputs are finite; a program needn't handle non-finite values.
Results may differ from the reference program's by a relative error of at most 0.012.
Values may be sent and summed in bfloat16 or wider, within the bound.
A program may use at most 128 MiB of HBM per device.

```python
import math
import jax
import jax.numpy as jnp
import numpy as np
from jax import lax

D = 2048
BLOCK = 256
BLOCKS = 8
TAPS = 4
FF = 3584
TOPK = 2
A_ROWS = 128
B_ROWS = 128
EXPERTS = 8
CAP = 40
TOK_A = 4096
TOK_B = 4096
N_TP = 4


def draw_decay_param(key, part):
    keys = jax.random.split(key, 3)
    fast = jax.random.uniform(keys[0], (D,), jnp.float32) < 0.5
    fast_rate = jnp.exp(jax.random.uniform(keys[1], (D,), jnp.float32, jnp.log(0.02), jnp.log(0.07)))
    slow_rate = jnp.exp(jax.random.uniform(keys[2], (D,), jnp.float32, jnp.log(0.2), jnp.log(1.0))) / TOK_A
    decay_rate = jnp.where(fast, fast_rate, slow_rate)
    return -jnp.log(jnp.expm1(decay_rate / 8.0))


def draw_decay_shift(key, part):
    keys = jax.random.split(key, 3)
    block_count = TOK_A // A_ROWS
    level = jnp.exp(jax.random.uniform(keys[0], (block_count,), jnp.float32, jnp.log(0.05), jnp.log(0.6))) / TOK_A
    shift_rows = -jnp.repeat(level, A_ROWS)
    spots = jax.random.randint(keys[1], (2,), 0, TOK_A)
    depth = jax.random.uniform(keys[2], (2,), jnp.float32, -0.5, -0.22)
    return shift_rows.at[spots].add(depth)


def levels(stream_key, dims, pieces, low, high):
    def one(position, shards_of):
        steps = jax.random.uniform(jax.random.fold_in(jax.random.fold_in(stream_key, 6), position), (shards_of,), jnp.float32, low / len(pieces), high / len(pieces))
        return jnp.repeat(jnp.exp(steps), dims[position] // shards_of).reshape((-1,) + (1,) * (len(dims) - position - 1))

    loudness = one(*pieces[0])
    for cut in pieces[1:]:
        loudness = loudness * one(*cut)
    return loudness


def shared_out(key, own, number, rows, amount, top, most, lean):
    order = jax.random.permutation(key, amount)
    packed, common = load_shares(amount, rows * top, most, lean, True), load_shares(amount, rows * top, most, lean, False)
    places = jnp.arange(amount)

    def named(sizes, turn):
        used = int((sizes > 0).sum())
        fixed = max(1, used // 4)
        moved = fixed + (places - fixed + turn * (used - fixed)) % max(1, amount - fixed)
        return jnp.zeros((amount,), jnp.int32).at[order[jnp.where(places < fixed, places, moved)]].set(jnp.asarray(sizes, jnp.int32))

    sizes = jnp.where(number % 4 == 0, named(packed, number // 4), named(common, number - number // 4 - 1))
    mixed = jax.random.permutation(jax.random.fold_in(own, 3), amount)
    donor, taker = mixed[0:amount // 2 * 2:2], mixed[1:amount // 2 * 2:2]
    margin = jnp.minimum(sizes[donor] - 1, most - sizes[taker]) // 2
    margin = jnp.where((donor == order[0]) | (taker == order[0]) | (sizes[taker] == 0), 0, jnp.maximum(margin, 0))
    moved = jax.random.randint(jax.random.fold_in(own, 4), (amount // 2,), 0, 1 << 20) % (margin + 1)
    sizes = sizes.at[donor].add(-moved).at[taker].add(moved)
    members = jnp.searchsorted(jnp.cumsum(sizes), jnp.arange(rows * top), side="right").astype(jnp.int32)
    listing = members.reshape(top, rows).T
    listing = listing[jax.random.permutation(jax.random.fold_in(own, 1), rows)]
    turn = jax.random.randint(jax.random.fold_in(own, 2), (rows, 1), 0, top)
    return jnp.take_along_axis(listing, (jnp.arange(top)[None, :] + turn) % top, axis=1)


def load_shares(amount, total, bound, skew, full):
    portions = [(1 << 20) // math.isqrt(grade ** skew) + 1 for grade in range(1, amount + 1)]
    largest = bound if full else min(bound, max(-(-total // amount), total * portions[0] // sum(portions)))
    least = 1 if total - largest >= amount - 1 else 0
    counts, surplus = [largest] + [least] * (amount - 1), total - largest - least * (amount - 1)
    while surplus > 0:
        movable = [i for i in range(1, amount) if counts[i] < largest] or [i for i in range(1, amount) if counts[i] < bound]
        mass, budget = sum([portions[i] for i in movable]), surplus
        for i in movable:
            addition = min(bound - counts[i], max(1, budget * portions[i] // mass), surplus)
            counts[i] = counts[i] + addition
            surplus = surplus - addition
    return np.array(counts)


def scatter_about(own_key, dims, width, most, cuts=(), kind=jnp.bfloat16):
    values = jax.random.normal(own_key, dims, jnp.float32) * width
    if len(cuts) > 0:
        values = levels(own_key, dims, cuts, -0.22, 0.18) * values
    return jnp.clip(values, min=-most, max=most).astype(kind)


def setup_inputs(seed: int = 0) -> dict:
    seeds = jax.random.split(jax.random.key(seed), 15)
    gate_branch = scatter_about(seeds[0], (TOK_A, D), 1.5, 8.0, ((0, 32),))
    rec_branch = scatter_about(seeds[1], (TOK_A, D), 1.0, 6.0, ((0, 32),))
    conv_weight = scatter_about(seeds[2], (TAPS, D), TAPS ** -0.5, 3.0, (), jnp.float32)
    gate_a = scatter_about(seeds[3], (BLOCKS, BLOCK, BLOCK), BLOCK ** -0.5, 0.375)
    gate_x = scatter_about(seeds[4], (BLOCKS, BLOCK, BLOCK), BLOCK ** -0.5, 0.375)
    decay_param = draw_decay_param(jax.random.fold_in(seeds[14], 71), 0)
    decay_shift = draw_decay_shift(jax.random.fold_in(seeds[14], 71), 0)
    tokens = scatter_about(seeds[7], (TOK_B, D), 1.0, 6.0, ((0, 32),))
    routes_keys = jax.random.split(jax.random.fold_in(seeds[8], 1), TOK_B // B_ROWS)
    routes_turns = jax.random.permutation(jax.random.fold_in(seeds[8], 3), TOK_B // B_ROWS)
    routes = jax.vmap(lambda own, number: shared_out(jax.random.fold_in(seeds[8], 2), own, number, B_ROWS, EXPERTS, TOPK, CAP, 2))(routes_keys, routes_turns).reshape((TOK_B, TOPK))
    route_weight = jnp.clip(0.1 + 0.79999997 * jax.random.uniform(seeds[9], (TOK_B, TOPK), jnp.float32) ** levels(seeds[9], (TOK_B, TOPK), ((0, 32),), -0.2, 0.2), 0.1, 0.9)
    norm_gain = jnp.clip(1.0 + 0.18 * jax.random.normal(seeds[10], (D,), jnp.float32), 0.1, 1.9)
    w_gate = scatter_about(seeds[11], (EXPERTS, D, FF), D ** -0.5, 0.125, ((0, 8), (2, 4)))
    w_up = scatter_about(seeds[12], (EXPERTS, D, FF), D ** -0.5, 0.125, ((0, 8), (2, 4)))
    w_down = scatter_about(seeds[13], (EXPERTS, FF, D), FF ** -0.5, 0.09375, ((0, 8), (1, 4)))
    return {"gate_branch": gate_branch, "rec_branch": rec_branch, "conv_weight": conv_weight, "gate_a": gate_a, "gate_x": gate_x, "decay_param": decay_param, "decay_shift": decay_shift, "tokens": tokens, "routes": routes, "route_weight": route_weight, "norm_gain": norm_gain, "w_gate": w_gate, "w_up": w_up, "w_down": w_down}


EPSILON = 1e-05

def pair_combine(earlier, later):
    return (earlier[0] * later[0], later[0] * earlier[1] + later[1])

def short_conv(previous, current, conv_weight):
    tap_count = conv_weight.shape[0]
    row_count = current.shape[0]
    padded = jnp.concatenate([previous, current], 0)
    summed = jnp.zeros(current.shape, jnp.float32)
    for tap_index in range(tap_count):
        summed = summed + conv_weight[tap_index] * padded[tap_index:tap_index + row_count].astype(jnp.float32)
    return summed.astype(jnp.bfloat16)

def mixer_gates(conv_rows, gate_a, gate_x, decay_rate, shift_rows):
    row_count, width_all = conv_rows.shape
    block_count, block_width = (gate_a.shape[0], gate_a.shape[1])
    split_rows = conv_rows.reshape(row_count, block_count, block_width).astype(jnp.float32)
    pre_a = jnp.einsum('rnc,ncd->rnd', split_rows, gate_a.astype(jnp.float32))
    pre_x = jnp.einsum('rnc,ncd->rnd', split_rows, gate_x.astype(jnp.float32))
    recur_gate = jax.nn.sigmoid(pre_a.reshape(row_count, width_all))
    input_gate = jax.nn.sigmoid(pre_x.reshape(row_count, width_all))
    log_a = -decay_rate[None, :] * recur_gate + shift_rows[:, None]
    drive = jnp.sqrt(-jnp.expm1(2.0 * log_a)) * input_gate * conv_rows.astype(jnp.float32)
    return (log_a, drive)

def mixer_reference(gate_branch, rec_branch, conv_weight, gate_a, gate_x, decay_param, decay_shift):
    total_rows, width_all = rec_branch.shape
    tap_count = conv_weight.shape[0]
    leading = jnp.zeros((tap_count - 1, width_all), jnp.bfloat16)
    conv_rows = short_conv(leading, rec_branch, conv_weight)
    decay_rate = 8.0 * jax.nn.softplus(-decay_param)
    span_rows = 512 if total_rows % 512 == 0 else total_rows
    span_count = total_rows // span_rows

    def advance(carried, span_index):
        start_row = span_index * span_rows
        conv_span = lax.dynamic_slice_in_dim(conv_rows, start_row, span_rows, 0)
        gate_span = lax.dynamic_slice_in_dim(gate_branch, start_row, span_rows, 0)
        shift_span = lax.dynamic_slice_in_dim(decay_shift, start_row, span_rows, 0)
        log_a, drive = mixer_gates(conv_span, gate_a, gate_x, decay_rate, shift_span)
        factor, local_state = lax.associative_scan(pair_combine, (jnp.exp(log_a), drive), axis=0)
        states = local_state + factor * carried[None, :]
        mixed = (states * jax.nn.gelu(gate_span.astype(jnp.float32), approximate=True)).astype(jnp.bfloat16)
        return (states[-1], mixed)
    start_state = jnp.zeros((width_all,), jnp.float32)
    _, mixed_spans = lax.scan(advance, start_state, jnp.arange(span_count, dtype=jnp.int32))
    return mixed_spans.reshape(total_rows, width_all)

def layer_scale(rows_in, norm_gain):
    values = rows_in.astype(jnp.float32)
    center = lax.optimization_barrier(jnp.mean(values, -1, keepdims=True))
    spread = lax.optimization_barrier(jnp.mean(jnp.square(values - center), -1, keepdims=True))
    return ((values - center) * lax.rsqrt(spread + EPSILON) * norm_gain).astype(jnp.bfloat16)

def slot_numbers(routes, block_rows, expert_count):
    row_count, top_count = routes.shape
    onehot = (routes[:, :, None] == jnp.arange(expert_count, dtype=jnp.int32)).astype(jnp.int32)
    ranked = jnp.cumsum(onehot.reshape(row_count // block_rows, block_rows * top_count, expert_count), axis=1) - 1
    return lax.optimization_barrier(jnp.sum(ranked.reshape(row_count, top_count, expert_count) * onehot, -1)).astype(jnp.int32)

def expert_result(rows_in, gate_full, up_full, down_full, shard_count):
    hidden = (jax.nn.silu(jnp.dot(rows_in, gate_full, preferred_element_type=jnp.float32)) * jnp.dot(rows_in, up_full, preferred_element_type=jnp.float32)).astype(jnp.bfloat16)
    unit_count = hidden.shape[1] // shard_count
    summed = jnp.zeros((rows_in.shape[0], down_full.shape[1]), jnp.float32)
    for shard_index in range(shard_count):
        lower = shard_index * unit_count
        piece = jnp.dot(hidden[:, lower:lower + unit_count], down_full[lower:lower + unit_count], preferred_element_type=jnp.float32).astype(jnp.bfloat16)
        piece = lax.optimization_barrier(piece)
        summed = summed + piece.astype(jnp.float32)
    return summed.astype(jnp.bfloat16)

def experts_reference(tokens, routes, route_weight, norm_gain, w_gate, w_up, w_down):
    row_count, width_all = tokens.shape
    expert_count = w_gate.shape[0]
    capacity = CAP
    block_count = row_count // B_ROWS
    normed = layer_scale(tokens, norm_gain)
    slots = slot_numbers(routes, B_ROWS, expert_count)
    row_ids = jnp.broadcast_to(jnp.arange(row_count, dtype=jnp.int32)[:, None], routes.shape)
    flat = (row_ids // B_ROWS * expert_count + routes) * capacity + slots
    table_size = block_count * expert_count * capacity
    table = jnp.full((table_size,), row_count, jnp.int32).at[flat.reshape(-1)].set(row_ids.reshape(-1))
    weight_table = jnp.zeros((table_size,), jnp.float32).at[flat.reshape(-1)].set(route_weight.reshape(-1))
    table = table.reshape(block_count, expert_count, capacity)
    weight_table = weight_table.reshape(block_count, expert_count, capacity)

    def add_expert(summed, expert_index):
        picks = jnp.take(table, expert_index, axis=1).reshape(-1)
        weights = jnp.take(weight_table, expert_index, axis=1).reshape(-1)
        rows_in = jnp.take(normed, picks, axis=0, mode='fill', fill_value=0)
        result = expert_result(rows_in, w_gate[expert_index], w_up[expert_index], w_down[expert_index], N_TP)
        summed = summed.at[picks].add(weights[:, None] * result.astype(jnp.float32), mode='drop')
        return (summed, None)
    start_sum = jnp.zeros((row_count, width_all), jnp.float32)
    summed, _ = lax.scan(add_expert, start_sum, jnp.arange(expert_count, dtype=jnp.int32))
    return summed.astype(jnp.bfloat16)

def reference(gate_branch, rec_branch, conv_weight, gate_a, gate_x, decay_param, decay_shift, tokens, routes, route_weight, norm_gain, w_gate, w_up, w_down):
    mixed_out = mixer_reference(gate_branch, rec_branch, conv_weight, gate_a, gate_x, decay_param, decay_shift)
    expert_out = experts_reference(tokens, routes, route_weight, norm_gain, w_gate, w_up, w_down)
    return (mixed_out, expert_out)
```

```python
import functools

import jax
import jax.numpy as jnp
from jax import lax
from jax.experimental import pallas as pl
from jax.experimental.pallas import tpu as pltpu
from jax.sharding import PartitionSpec as P

EPSILON = 1e-05
MESH = pl.DeviceIdType.MESH


def passed_along(block, axis, distance):
    devices = range(lax.axis_size(axis))
    route = [(i - distance, i) for i in devices if i - distance in devices]
    return lax.ppermute(block, axis, route)


def slot_numbers(routes, block_rows, expert_count):
    row_count, top_count = routes.shape
    onehot = (routes[:, :, None] == jnp.arange(expert_count, dtype=jnp.int32)).astype(jnp.int32)
    ranked = (
        jnp.cumsum(
            onehot.reshape(row_count // block_rows, block_rows * top_count, expert_count), axis=1
        )
        - 1
    )
    return jnp.sum(ranked.reshape(row_count, top_count, expert_count) * onehot, -1)


def shifted(values, distance, fill):
    lead = jnp.full((distance, values.shape[1]), fill, values.dtype)
    return jnp.concatenate([lead, values[: values.shape[0] - distance]], 0)


def mixer_kernel(prev_ref, rec_ref, conv_ref, ga_ref, gx_ref, rate_ref, shift_ref, f_ref, s_ref):
    rows = rec_ref.shape[0]
    taps = conv_ref.shape[0]
    lead = prev_ref.shape[0]
    padded = jnp.concatenate([prev_ref[...], rec_ref[...].astype(jnp.float32)], 0)
    first = lead - (taps - 1)
    summed = jnp.zeros(rec_ref.shape, jnp.float32)
    for tap in range(taps):
        summed = summed + conv_ref[tap : tap + 1, :] * padded[first + tap : first + tap + rows]
    conv_rows = summed.astype(jnp.bfloat16)
    recur = jax.nn.sigmoid(jnp.dot(conv_rows, ga_ref[0], preferred_element_type=jnp.float32))
    gate = jax.nn.sigmoid(jnp.dot(conv_rows, gx_ref[0], preferred_element_type=jnp.float32))
    log_a = -rate_ref[...] * recur + shift_ref[...]
    twice = 2.0 * log_a
    series = twice * (1.0 + twice * (0.5 + twice * (1.0 / 6.0 + twice * (1.0 / 24.0))))
    lost = jnp.where(twice > -0.03, -series, 1.0 - jnp.exp(twice))
    state = jnp.sqrt(lost) * gate * conv_rows.astype(jnp.float32)
    factor = jnp.exp(log_a)
    distance = 1
    while distance < rows:
        state = factor * shifted(state, distance, 0.0) + state
        factor = factor * shifted(factor, distance, 1.0)
        distance *= 2
    f_ref[...] = factor
    s_ref[...] = state


def local_mixer(prev, rec, conv_weight, gate_a, gate_x, rate, shift):
    rows, width = rec.shape
    blocks, wide = gate_a.shape[:2]
    col = lambda r: pl.BlockSpec((r, wide), lambda i: (0, i))
    mat = pl.BlockSpec((1, wide, wide), lambda i: (i, 0, 0))
    return pl.pallas_call(
        mixer_kernel,
        grid=(blocks,),
        in_specs=[col(prev.shape[0]), col(rows), col(conv_weight.shape[0]), mat, mat, col(1),
                  pl.BlockSpec((rows, 1), lambda i: (0, 0))],
        out_specs=[col(rows), col(rows)],
        out_shape=[jax.ShapeDtypeStruct((rows, width), jnp.float32)] * 2,
    )(prev, rec, conv_weight, gate_a, gate_x, rate, shift)


def expert_kernel(n, m, slot, tok_ref, gain_ref, flat_ref, flat_t_ref, weight_ref, tot_ref,
                  wg_hbm, wu_hbm, wd_hbm, out_ref, carry_ref,
                  wg, wu, wd, going, rows, half, back, tp_tot, grp, ep_tot,
                  w_sem, d_s, d_r, a_s, a_r, b_s, b_r, c_s, c_r, ra_s, ra_r, rb_s, rb_r,
                  q_s, q_r, t_s, t_r, e_s, e_r):
    e = lax.axis_index("ep")
    t = lax.axis_index("tp")
    pa = t + 1 - 2 * (t % 2)
    pb = (t + m // 2) % m
    pd = (pa + m // 2) % m
    loads = [pltpu.make_async_copy(h, v, w_sem.at[i])
             for i, (h, v) in enumerate(((wg_hbm, wg), (wu_hbm, wu), (wd_hbm, wd)))]
    for load in loads:
        load.start()

    barrier = pltpu.get_barrier_semaphore()

    def greet(k, _):
        pl.semaphore_signal(barrier, inc=1, device_id=((e + k) % n, t), device_id_type=MESH)
        return 0

    lax.fori_loop(1, n, greet, 0)
    for d in range(1, m):
        pl.semaphore_signal(barrier, inc=1, device_id=(e, (t + d) % m), device_id_type=MESH)

    def at(r, s, q):
        return r.at[s, pl.ds(pl.multiple_of(q * slot, slot), slot), :]

    def part(s, q):
        return rows[s, pl.ds(pl.multiple_of(q * slot, slot), slot), :].astype(jnp.float32)

    def remote(src, dst, s, r, device):
        return pltpu.make_async_remote_copy(src_ref=src, dst_ref=dst, send_sem=s, recv_sem=r,
                                            device_id=device, device_id_type=MESH)

    def send_d(k):
        return remote(going.at[(e + n - k) % n], at(rows, e, t), d_s.at[k], d_r.at[k],
                      ((e + n - k) % n, t))

    def send_a(k):
        s = (e + k) % n
        return remote(at(rows, s, t), at(rows, s, t), a_s.at[k], a_r.at[k], (e, pa))

    def send_b(k):
        s = (e + k) % n
        return remote(at(rows, s, t), at(rows, s, t), b_s.at[k], b_r.at[k], (e, pb))

    def send_c(k):
        s = (e + k) % n
        return remote(at(rows, s, pb), at(rows, s, pb), c_s.at[k], c_r.at[k], (e, pa))

    def send_ra(k, j):
        s = (e + k) % n
        return remote(at(rows, s, pa if j == 0 else pd), half.at[k, j], ra_s.at[k, j],
                      ra_r.at[k, j], (e, pa))

    def send_rb(k):
        return remote(half.at[k, 1], half.at[k, 2], rb_s.at[k], rb_r.at[k], (e, pb))

    def send_q(k):
        return remote(half.at[k, 0], back.at[e], q_s.at[k], q_r.at[k], ((e + k) % n, t))

    def send_t(d):
        return remote(tot_ref, tp_tot.at[t], t_s.at[d], t_r.at[d], (e, (t + d) % m))

    def send_e(k):
        return remote(grp, ep_tot.at[e], e_s.at[k], e_r.at[k], ((e + k) % n, t))

    values = tok_ref[...].astype(jnp.float32)
    center = jnp.mean(values, -1, keepdims=True)
    spread = jnp.mean(jnp.square(values - center), -1, keepdims=True)
    normed = ((values - center) * lax.rsqrt(spread + EPSILON) * gain_ref[...]).astype(jnp.bfloat16)
    count = values.shape[0]
    top = flat_ref.shape[0]
    place = lax.broadcasted_iota(jnp.int32, (n * slot, count), 0)
    pick = jnp.zeros((n * slot, count), jnp.float32)
    for k in range(top):
        pick = pick + jnp.where(place == flat_ref[k : k + 1, :], 1.0, 0.0)
    outgoing = jnp.dot(pick.astype(jnp.bfloat16), normed, preferred_element_type=jnp.float32)
    going[...] = outgoing.astype(jnp.bfloat16).reshape(going.shape)
    rows[e, pl.ds(pl.multiple_of(t * slot, slot), slot), :] = going[e]
    tp_tot[t] = tot_ref[...]

    pl.semaphore_wait(barrier, n - 1 + m - 1)

    def go(k, _):
        send_d(k).start()
        return 0

    for d in range(1, m):
        send_t(d).start()
    lax.fori_loop(1, n, go, 0)

    for d in range(1, m):
        send_t(d).wait_recv()
    total_f = tp_tot[0, 0:1, :]
    total_s = tp_tot[0, 1:2, :]
    for d in range(1, m):
        total_s = tp_tot[d, 0:1, :] * total_s + tp_tot[d, 1:2, :]
        total_f = total_f * tp_tot[d, 0:1, :]
    grp[0:1, :] = total_f
    grp[1:2, :] = total_s
    grp[2:, :] = jnp.zeros((grp.shape[0] - 2, grp.shape[1]), jnp.float32)
    ep_tot[e] = grp[...]

    def go_e(k, _):
        send_e(k).start()
        return 0

    lax.fori_loop(1, n, go_e, 0)
    for load in loads:
        load.wait()

    def step(i, _):
        @pl.when(i < n)
        def _():
            @pl.when(i > 0)
            def _():
                send_d(i).wait_recv()

            send_b(i).start()
            send_a(i).start()

        @pl.when((i >= 1) & (i < n + 1))
        def _():
            k = i - 1
            send_b(k).wait_recv()
            send_c(k).start()

        @pl.when((i >= 2) & (i < n + 2))
        def _():
            k = i - 2
            s = (e + k) % n
            send_a(k).wait_recv()
            send_c(k).wait_recv()
            x = rows[s]
            hidden = (jax.nn.silu(jnp.dot(x, wg[...], preferred_element_type=jnp.float32))
                      * jnp.dot(x, wu[...], preferred_element_type=jnp.float32)).astype(jnp.bfloat16)
            result = jnp.dot(hidden, wd[...], preferred_element_type=jnp.float32)
            send_a(k).wait_send()
            send_b(k).wait_send()
            send_c(k).wait_send()
            rows[s] = result.astype(jnp.bfloat16)
            send_ra(k, 1).start()
            send_ra(k, 0).start()

        @pl.when((i >= 3) & (i < n + 3))
        def _():
            k = i - 3
            s = (e + k) % n
            send_ra(k, 1).wait_recv()
            both = part(s, pb) + half[k, 1].astype(jnp.float32)
            half[k, 1] = both.astype(jnp.bfloat16)
            send_rb(k).start()

        @pl.when(i >= 4)
        def _():
            k = i - 4
            s = (e + k) % n
            send_ra(k, 0).wait_recv()
            send_rb(k).wait_recv()
            whole = part(s, t) + half[k, 0].astype(jnp.float32) + half[k, 2].astype(jnp.float32)
            half[k, 0] = whole.astype(jnp.bfloat16)

            @pl.when(k > 0)
            def _():
                send_q(k).start()

            @pl.when(k == 0)
            def _():
                back[e] = whole.astype(jnp.bfloat16)

        return 0

    lax.fori_loop(0, n + 4, step, 0)

    def finish(k, _):
        send_d(k).wait_send()
        send_e(k).wait()
        send_q(k).wait()
        return 0

    lax.fori_loop(1, n, finish, 0)

    def finish_local(k, _):
        send_ra(k, 0).wait_send()
        send_ra(k, 1).wait_send()
        send_rb(k).wait_send()
        return 0

    lax.fori_loop(0, n, finish_local, 0)
    for d in range(1, m):
        send_t(d).wait_send()

    carried = jnp.zeros((1, grp.shape[1]), jnp.float32)

    def over(k, carried):
        new = ep_tot[k, 0:1, :] * carried + ep_tot[k, 1:2, :]
        return jnp.where(k < e, new, carried)

    carried = lax.fori_loop(0, n, over, carried)
    for d in range(m):
        new = tp_tot[d, 0:1, :] * carried + tp_tot[d, 1:2, :]
        carried = jnp.where(d < t, new, carried)
    carry_ref[...] = jnp.broadcast_to(carried, carry_ref.shape)

    results = back[...].reshape(n * slot, back.shape[2])
    place = lax.broadcasted_iota(jnp.int32, (count, n * slot), 1)
    summed = jnp.zeros(out_ref.shape, jnp.float32)
    for k in range(top):
        pick = jnp.where(place == flat_t_ref[:, k : k + 1], 1.0, 0.0).astype(jnp.bfloat16)
        picked = jnp.dot(pick, results, preferred_element_type=jnp.float32)
        summed = summed + picked * weight_ref[:, k : k + 1]
    out_ref[...] = summed.astype(jnp.bfloat16)


def experts(n, m, slot, tokens, gain, flat, route_weight, totals, w_gate, w_up, w_down):
    count, width = tokens.shape
    hidden = w_gate.shape[1]
    dma = lambda *shape: pltpu.SemaphoreType.DMA(shape)
    vmem = pl.BlockSpec(memory_space=pltpu.VMEM)
    anyw = pl.BlockSpec(memory_space=pl.ANY)
    bf = jnp.bfloat16
    return pl.pallas_call(
        functools.partial(expert_kernel, n, m, slot),
        in_specs=[vmem] * 6 + [anyw] * 3,
        out_specs=[vmem] * 2,
        out_shape=[jax.ShapeDtypeStruct((count, width), bf), jax.ShapeDtypeStruct((8, width), jnp.float32)],
        scratch_shapes=[
            pltpu.VMEM((width, hidden), bf), pltpu.VMEM((width, hidden), bf),
            pltpu.VMEM((hidden, width), bf),
            pltpu.VMEM((n, slot, width), bf), pltpu.VMEM((n, m * slot, width), bf),
            pltpu.VMEM((n, 3, slot, width), bf), pltpu.VMEM((n, slot, width), bf),
            pltpu.VMEM((m, 8, width), jnp.float32), pltpu.VMEM((8, width), jnp.float32),
            pltpu.VMEM((n, 8, width), jnp.float32),
            dma(3)] + [dma(n)] * 8 + [dma(n, 2)] * 2 + [dma(n)] * 4 + [dma(m)] * 2 + [dma(n)] * 2,
        compiler_params=pltpu.CompilerParams(
            collective_id=0, has_side_effects=True, vmem_limit_bytes=63 * 1024 * 1024),
    )(tokens, gain, flat.T, flat, route_weight, totals, w_gate, w_up, w_down)


def shards(
    gate_branch,
    rec_branch,
    conv_weight,
    gate_a,
    gate_x,
    decay_param,
    decay_shift,
    tokens,
    routes,
    route_weight,
    norm_gain,
    w_gate,
    w_up,
    w_down,
):
    tap_count = conv_weight.shape[0]
    row_count, width_all = rec_branch.shape
    n, m = lax.axis_size("ep"), lax.axis_size("tp")
    previous = passed_along(rec_branch[row_count - (tap_count - 1) :], ("ep", "tp"), 1)
    lead = -(tap_count - 1) % 8
    previous = jnp.pad(previous.astype(jnp.float32), ((lead, 0), (0, 0)))
    rate = 8.0 * jax.nn.softplus(-decay_param)
    factor, state = local_mixer(
        previous, rec_branch, conv_weight, gate_a, gate_x, rate[None, :], decay_shift[:, None]
    )
    totals = jnp.concatenate(
        [factor[-1:], state[-1:], jnp.zeros((6, width_all), jnp.float32)], 0
    )
    block_rows, top_count = routes.shape
    capacity = max(2, block_rows * top_count * 5 // (4 * n))
    slot = -(-capacity // 16) * 16
    flat = routes * slot + slot_numbers(routes, block_rows, n)
    expert_out, carried = experts(
        n, m, slot, tokens, norm_gain[None, :], flat, route_weight, totals,
        w_gate[0], w_up[0], w_down[0],
    )
    states = state + factor * carried[0:1]
    mixed_out = (states * jax.nn.gelu(gate_branch.astype(jnp.float32), approximate=True)).astype(
        jnp.bfloat16
    )
    return (mixed_out, expert_out)


def solution(mesh):
    in_specs = (
        P(("ep", "tp"), None),
        P(("ep", "tp"), None),
        P(),
        P(),
        P(),
        P(),
        P(("ep", "tp")),
        P(("ep", "tp"), None),
        P(("ep", "tp"), None),
        P(("ep", "tp"), None),
        P(),
        P("ep", None, "tp"),
        P("ep", None, "tp"),
        P("ep", "tp", None),
    )
    out_specs = (P(("ep", "tp"), None), P(("ep", "tp"), None))
    return jax.shard_map(shards, mesh=mesh, in_specs=in_specs, out_specs=out_specs, check_vma=False)
```
